256 devices in a mesh: ep: 16 (over y, x), tp: 16 (over z, core).
Axes of the slice: x: 4, y: 4, z: 8, core: 2. Of those that a mesh axis runs over, the one named last changes fastest.
Arguments:
- tokens: bfloat16 [256, 4096], P(None, 'ep'), may hold values from -60 to 60
- gain_attn: bfloat16 [4096], P('ep'), may hold values from 0.099609375 to 1.8984375
- w_query: bfloat16 [4096, 2048], P('ep', 'tp'), may hold values from -0.09375 to 0.09375
- w_key: bfloat16 [4096, 2048], P('ep', 'tp'), may hold values from -0.09375 to 0.09375
- w_value: bfloat16 [4096, 2048], P('ep', 'tp'), may hold values from -0.09375 to 0.09375
- w_output: bfloat16 [2048, 4096], P('tp', 'ep'), may hold values from -0.125 to 0.125
- key_cache: bfloat16 [256, 1024, 2048], P('ep', None, 'tp'), may hold values from -6 to 6
- value_cache: bfloat16 [256, 1024, 2048], P('ep', None, 'tp'), may hold values from -10 to 10
- lengths: int32 [256], P('ep'), may hold values from 128 to 1024
- score_shift: float32 [16], P('tp'), may hold values from -9.5 to -3.5
- gain_ffn: bfloat16 [4096], replicated, may hold values from 0.099609375 to 1.8984375
- w_mix: bfloat16 [4096], P('ep'), may hold values from -0.09375 to 0.09375
- w_dense_gate: bfloat16 [4096, 4096], P('ep', 'tp'), may hold values from -0.09375 to 0.09375
- w_dense_up: bfloat16 [4096, 4096], P('ep', 'tp'), may hold values from -0.09375 to 0.09375
- w_dense_down: bfloat16 [4096, 4096], P('tp', 'ep'), may hold values from -0.09375 to 0.09375
- route_group: int32 [256], replicated, may hold values from 0 to 3, as said below
- route_inner: int32 [256, 2], replicated, may hold values from 0 to 3, as said below
- route_weight: float32 [256, 2], replicated, may hold values from 0.3 to 1
- w_exp_gate: bfloat16 [16, 4096, 2048], P('ep', None, 'tp'), may hold values from -0.09375 to 0.09375
- w_exp_up: bfloat16 [16, 4096, 2048], P('ep', None, 'tp'), may hold values from -0.09375 to 0.09375
- w_exp_down: bfloat16 [16, 2048, 4096], P('ep', 'tp'), may hold values from -0.125 to 0.125
Outputs:
- mixed: bfloat16 [256, 4096], P(None, 'ep')
- new_keys: bfloat16 [256, 2048], P('ep', 'tp')
- new_values: bfloat16 [256, 2048], P('ep', 'tp')
The draws below stay inside these ranges and needn't reach their ends.
Inputs may be any that keep to these rules, and one draw needn't show every extreme that they name: `route_group`: within every aligned block of 16 sequences (the sequences of one index of ep) exactly half of the tokens use one group, the same group in every block; the other groups share the rest. A token's 2 experts inside its group differ. Within every aligned block of 16 sequences no expert (route_group * 4 + route_inner) is used by more than 4 tokens, and the experts of the group that half of the block uses are each used by exactly 4.
All inputs are finite; a program needn't handle non-finite values.
Results may differ from the reference program's by a relative error of at most 0.0039.
The reference program's roundings to bfloat16 on the way count: a program that leaves them out, or rounds other values in their place, can miss the bound.
Values may be sent and summed in bfloat16 or wider, within the bound.
A program may use at most 64 MiB of HBM per device.

```python
import math
import jax
import jax.numpy as jnp
from jax import lax

D = 4096
HEADS = 16
HD = 128
FF = 2048
FFD = 4096
GROUPS = 4
EPG = 4
TOPK = 2
SEQ_DEV = 16
CACHE_LEN = 1024
BATCH = 256
EXPERTS = 16
ATT = 2048
N_EP = 16


def draw_tokens(key, part):
    column_block = jnp.arange(D) // (D // N_EP)
    rising = jnp.exp(jnp.log(3.0) * column_block / max(N_EP - 1, 1))
    base_part = jnp.clip(jax.random.normal(key, (BATCH, D), jnp.float32), -6.0, 6.0)
    return (base_part * rising[None, :]).astype(jnp.bfloat16)


def draw_value_cache(key, part):
    common = jnp.clip(jax.random.normal(jax.random.fold_in(key, 3), (BATCH, 1, ATT), jnp.float32), -5.0, 5.0)
    fresh_part = jnp.clip(jax.random.normal(jax.random.fold_in(key, 4), (BATCH, CACHE_LEN, ATT), jnp.float32), -5.0, 5.0)
    return (0.8 * common + 0.6 * fresh_part).astype(jnp.bfloat16)


def draw_score_shift(key, part):
    return jax.random.uniform(key, (HEADS,), jnp.float32, -9.0, -3.5)


def shuffle_many(subkeys, length):

    def shuffle_one(subkey):
        return jax.random.permutation(subkey, length)
    return jax.vmap(shuffle_one)(subkeys)


def route_table(key):
    base_key = jax.random.fold_in(key, 17)
    blocks = BATCH // SEQ_DEV
    half_block = SEQ_DEV // 2
    favored = jax.random.randint(jax.random.fold_in(base_key, 1), (), 0, GROUPS)
    first_share = jax.random.randint(jax.random.fold_in(base_key, 2), (blocks,), 0, half_block + 1)
    second_share = jax.random.randint(jax.random.fold_in(base_key, 3), (blocks,), 0, half_block + 1 - first_share)
    rotation = jax.random.randint(jax.random.fold_in(base_key, 4), (blocks,), 0, 3)
    position = jnp.arange(SEQ_DEV)[None, :]
    remaining = position - half_block
    other_slot = jnp.where(remaining < first_share[:, None], 0, jnp.where(remaining < first_share[:, None] + second_share[:, None], 1, 2))
    group_label = jnp.where(position < half_block, favored, (favored + 1 + (other_slot + rotation[:, None]) % 3) % GROUPS)
    shuffle_order = shuffle_many(jax.random.split(jax.random.fold_in(base_key, 5), blocks), SEQ_DEV)
    group_of = jnp.take_along_axis(group_label, shuffle_order, axis=1)
    same_group = (group_of[:, :, None] == jnp.arange(GROUPS)[None, None, :]).astype(jnp.int32)
    before = jnp.cumsum(same_group, axis=1) - same_group
    slot_rank = jnp.sum(before * same_group, axis=2)
    cycles = shuffle_many(jax.random.split(jax.random.fold_in(base_key, 6), blocks * GROUPS), EPG).reshape(blocks, GROUPS, EPG)
    cycle_of = jnp.sum(same_group[:, :, :, None] * cycles[:, None, :, :], axis=2)
    inner_range = jnp.arange(EPG)[None, None, :]
    first_pick = jnp.sum(cycle_of * (inner_range == (slot_rank % EPG)[:, :, None]), axis=2)
    second_pick = jnp.sum(cycle_of * (inner_range == ((slot_rank + 1) % EPG)[:, :, None]), axis=2)
    inner_pick = jnp.stack([first_pick, second_pick], axis=2).reshape(BATCH, 2)
    return (group_of.reshape(BATCH).astype(jnp.int32), inner_pick.astype(jnp.int32))


def draw_route_group(key, part):
    return route_table(key)[0]


def draw_route_inner(key, part):
    return route_table(key)[1]


def set_ends(array, stream_key, smallest, high):
    spot = [jax.random.randint(jax.random.fold_in(stream_key, axis), (), 0, length) for axis, length in enumerate(array.shape)]
    main_axis = array.shape.index(max(array.shape))
    next_to = spot[:main_axis] + [(spot[main_axis] + 1) % array.shape[main_axis]] + spot[main_axis + 1:]
    return array.at[tuple(spot)].set(smallest).at[tuple(next_to)].set(high)


def steps_of(stream_key, dims, cuts, low, top_value):
    def one(axis_at, shards_of):
        draws = jax.random.uniform(jax.random.fold_in(jax.random.fold_in(stream_key, 6), axis_at), (shards_of,), jnp.float32, low / len(cuts), top_value / len(cuts))
        return jnp.repeat(jnp.exp(draws), dims[axis_at] // shards_of).reshape((-1,) + (1,) * (len(dims) - axis_at - 1))

    gain = one(*cuts[0])
    for cut in cuts[1:]:
        gain = gain * one(*cut)
    return gain


def normal_values(key, dims, width, reach, cuts=(), kind=jnp.bfloat16):
    drawn = width * jax.random.normal(key, dims, jnp.float32)
    if cuts:
        drawn = drawn * steps_of(key, dims, cuts, -0.22, 0.18)
    return jnp.clip(drawn, -reach, reach).astype(kind)


def setup_inputs(seed: int = 0) -> dict:
    keys = jax.random.split(jax.random.key(seed), 22)
    tokens = draw_tokens(jax.random.fold_in(keys[21], 71), 0)
    gain_attn = jnp.clip(1.0 + 0.18 * jax.random.normal(keys[1], (D,), jnp.float32), 0.099609375, 1.8984375).astype(jnp.bfloat16)
    w_query = normal_values(keys[2], (D, ATT), D ** -0.5, 0.09375, ((0, 16), (1, 16)))
    w_key = normal_values(keys[3], (D, ATT), D ** -0.5, 0.09375, ((0, 16), (1, 16)))
    w_value = normal_values(keys[4], (D, ATT), D ** -0.5, 0.09375, ((0, 16), (1, 16)))
    w_output = normal_values(keys[5], (ATT, D), ATT ** -0.5, 0.125, ((0, 16), (1, 16)))
    key_cache = normal_values(keys[6], (BATCH, CACHE_LEN, ATT), 1.0, 6.0, ((0, 16), (2, 16)))
    value_cache = draw_value_cache(jax.random.fold_in(keys[21], 71), 0)
    lengths = set_ends(jax.random.randint(keys[8], (BATCH,), CACHE_LEN // 8, CACHE_LEN + 1), jax.random.fold_in(keys[8], 1), CACHE_LEN // 8, CACHE_LEN).astype(jnp.int32)
    score_shift = draw_score_shift(jax.random.fold_in(keys[21], 71), 0)
    gain_ffn = jnp.clip(1.0 + 0.18 * jax.random.normal(keys[10], (D,), jnp.float32), 0.099609375, 1.8984375).astype(jnp.bfloat16)
    w_mix = normal_values(keys[11], (D,), D ** -0.5, 0.09375, ((0, 16),))
    w_dense_gate = normal_values(keys[12], (D, FFD), D ** -0.5, 0.09375, ((0, 16), (1, 16)))
    w_dense_up = normal_values(keys[13], (D, FFD), D ** -0.5, 0.09375, ((0, 16), (1, 16)))
    w_dense_down = normal_values(keys[14], (FFD, D), FFD ** -0.5, 0.09375, ((0, 16), (1, 16)))
    route_group = draw_route_group(jax.random.fold_in(keys[21], 71), 0)
    route_inner = draw_route_inner(jax.random.fold_in(keys[21], 71), 0)
    route_weight = jnp.clip(jax.random.uniform(keys[17], (BATCH, TOPK), jnp.float32, 0.3, 1.0), 0.3, 1.0)
    w_exp_gate = normal_values(keys[18], (EXPERTS, D, FF), D ** -0.5, 0.09375, ((0, 16), (2, 16)))
    w_exp_up = normal_values(keys[19], (EXPERTS, D, FF), D ** -0.5, 0.09375, ((0, 16), (2, 16)))
    w_exp_down = normal_values(keys[20], (EXPERTS, FF, D), FF ** -0.5, 0.125, ((0, 16), (1, 16)))
    return {"tokens": tokens, "gain_attn": gain_attn, "w_query": w_query, "w_key": w_key, "w_value": w_value, "w_output": w_output, "key_cache": key_cache, "value_cache": value_cache, "lengths": lengths, "score_shift": score_shift, "gain_ffn": gain_ffn, "w_mix": w_mix, "w_dense_gate": w_dense_gate, "w_dense_up": w_dense_up, "w_dense_down": w_dense_down, "route_group": route_group, "route_inner": route_inner, "route_weight": route_weight, "w_exp_gate": w_exp_gate, "w_exp_up": w_exp_up, "w_exp_down": w_exp_down}


norm_eps = 1e-06

def reference(tokens, gain_attn, w_query, w_key, w_value, w_output, key_cache, value_cache, lengths, score_shift, gain_ffn, w_mix, w_dense_gate, w_dense_up, w_dense_down, route_group, route_inner, route_weight, w_exp_gate, w_exp_up, w_exp_down):
    tokens_float = tokens.astype(jnp.float32)
    inv_first = lax.rsqrt(lax.optimization_barrier(jnp.mean(tokens_float * tokens_float, axis=1, keepdims=True)) + norm_eps)
    scaled_in = (tokens_float * gain_attn.astype(jnp.float32)).astype(jnp.bfloat16)
    queries = (jnp.dot(scaled_in, w_query, preferred_element_type=jnp.float32) * inv_first).astype(jnp.bfloat16)
    new_keys = (jnp.dot(scaled_in, w_key, preferred_element_type=jnp.float32) * inv_first).astype(jnp.bfloat16)
    new_values = (jnp.dot(scaled_in, w_value, preferred_element_type=jnp.float32) * inv_first).astype(jnp.bfloat16)

    def attend_block(inputs):
        block_query, block_keys, block_values, block_lengths = inputs
        seq_count = block_query.shape[0]
        head_query = block_query.astype(jnp.float32).reshape(seq_count, HEADS, HD)
        head_keys = block_keys.astype(jnp.float32).reshape(seq_count, CACHE_LEN, HEADS, HD)
        scores = jnp.einsum('bhd,blhd->bhl', head_query, head_keys) / math.sqrt(HD) + score_shift[None, :, None]
        position = jnp.arange(CACHE_LEN, dtype=jnp.int32)
        live_mask = position[None, None, :] < block_lengths[:, None, None]
        soft_terms = jnp.where(live_mask, jax.nn.softplus(scores), 0.0)
        later_sum = lax.cumsum(soft_terms, axis=2, reverse=True) - soft_terms
        stick = jnp.where(live_mask, jnp.exp(jax.nn.log_sigmoid(scores) - later_sum), 0.0)
        stick = lax.optimization_barrier(stick.astype(jnp.bfloat16)).astype(jnp.float32)
        head_values = block_values.astype(jnp.float32).reshape(seq_count, CACHE_LEN, HEADS, HD)
        attended = jnp.einsum('bhl,blhd->bhd', stick, head_values)
        return attended.reshape(seq_count, ATT).astype(jnp.bfloat16)
    block_count = BATCH // SEQ_DEV
    attended = lax.map(attend_block, (queries.reshape(block_count, SEQ_DEV, ATT), key_cache.reshape(block_count, SEQ_DEV, CACHE_LEN, ATT), value_cache.reshape(block_count, SEQ_DEV, CACHE_LEN, ATT), lengths.reshape(block_count, SEQ_DEV))).reshape(BATCH, ATT)
    attn_out = jnp.dot(attended, w_output, preferred_element_type=jnp.float32)
    middle = (tokens_float + attn_out).astype(jnp.bfloat16)
    middle_float = middle.astype(jnp.float32)
    inv_second = lax.rsqrt(lax.optimization_barrier(jnp.mean(middle_float * middle_float, axis=1, keepdims=True)) + norm_eps)
    scaled_mid = (middle_float * gain_ffn.astype(jnp.float32)).astype(jnp.bfloat16)
    dense_pre = jnp.dot(scaled_mid, w_dense_gate, preferred_element_type=jnp.float32) * inv_second
    dense_lin = jnp.dot(scaled_mid, w_dense_up, preferred_element_type=jnp.float32) * inv_second
    dense_hidden = (jax.nn.silu(dense_pre) * dense_lin).astype(jnp.bfloat16)
    mix_gate = jax.nn.sigmoid(jnp.dot(scaled_mid, w_mix, preferred_element_type=jnp.float32) * inv_second[:, 0])
    dense_out = jnp.dot(dense_hidden, w_dense_down, preferred_element_type=jnp.float32) * mix_gate[:, None]
    expert_ids = (route_group[:, None] * EPG + route_inner).astype(jnp.int32)
    expert_range = jnp.arange(EXPERTS, dtype=jnp.int32)
    combine = lax.optimization_barrier(jnp.sum(jnp.where(expert_ids[:, :, None] == expert_range[None, None, :], route_weight[:, :, None], 0.0), axis=1))

    def add_expert(running, expert_index):
        gate_pre = jnp.dot(scaled_mid, w_exp_gate[expert_index], preferred_element_type=jnp.float32) * inv_second
        up_proj = jnp.dot(scaled_mid, w_exp_up[expert_index], preferred_element_type=jnp.float32) * inv_second
        hidden = (jax.nn.silu(gate_pre) * up_proj).astype(jnp.bfloat16)
        output_rows = jnp.dot(hidden, w_exp_down[expert_index], preferred_element_type=jnp.float32)
        weight_col = lax.dynamic_index_in_dim(combine, expert_index, 1, keepdims=True)
        return (running + output_rows * weight_col, None)
    expert_total, _ = lax.scan(add_expert, jnp.zeros((BATCH, D), jnp.float32), expert_range)
    mixed = (middle_float + expert_total + dense_out).astype(jnp.bfloat16)
    return (mixed, new_keys, new_values)
```

```python
import functools
import math

import jax
import jax.numpy as jnp
from jax import lax
from jax.experimental import pallas as pl
from jax.experimental.pallas import tpu as pltpu
from jax.sharding import PartitionSpec as P

MESH = pl.DeviceIdType.MESH
HD = 128
EPG = 4
CAP = 4
EPS = 1e-06
F32 = jnp.float32
BF16 = jnp.bfloat16

QP, KVP, ATT, AOUT, MID, DISP, DENSE, DHID, RET, FIN, OUT = range(11)
N_PHASE = 11
VMEM_BYTES = 67_043_328


def dot(a, b):
    return jnp.dot(a, b, preferred_element_type=F32)


def dot_nt(a, b):
    return lax.dot_general(a, b, (((1,), (1,)), ((), ())), preferred_element_type=F32)


def hi_lo(col, width):
    rows = col.shape[0]
    hi = col.astype(BF16).astype(F32)
    lane = lax.broadcasted_iota(jnp.int32, (rows, width), 1)
    return jnp.where(lane < width // 2, hi, col - hi)


def un_hi_lo(pair):
    half = pair.shape[1] // 2
    return pair[:, 0:1] + pair[:, half : half + 1]


def layer(
    n_ep,
    n_tp,
    depth_all,
    tokens,
    gain,
    wq,
    wk,
    wv,
    wo,
    kc,
    vc,
    lengths,
    shift,
    gffn_row,
    wmix,
    wdg,
    wdu,
    wdd,
    rg,
    ri,
    rw,
    weg,
    weu,
    wed,
    mixed_out,
    nk_out,
    nv_out,
    tok_v,
    wq_v,
    wk_v,
    wv_v,
    wo_v,
    k_v,
    v_v,
    wdg_v,
    wdu_v,
    wdd_v,
    weg_v,
    weu_v,
    wed_v,
    onehot_v,
    combine_v,
    q_s,
    q_r,
    kv_s,
    kv_r,
    att_s,
    att_r,
    ao_s,
    ao_r,
    mid_s,
    mid_r,
    disp_s,
    disp_r,
    den_s,
    den_r,
    dh_s,
    dh_r,
    ret_s,
    ret_r,
    fin_s,
    fin_r,
    out_s,
    out_r,
    load_sem,
    send_sem,
    recv_sem,
):
    e = lax.axis_index("ep")
    t = lax.axis_index("tp")
    batch, width = tok_v.shape
    seqs = batch // n_ep
    tb = batch // n_tp
    slots = CAP * n_ep
    cache_len = k_v.shape[1]

    barrier = pltpu.get_barrier_semaphore()

    def greet(d, _):
        pl.semaphore_signal(barrier, inc=1, device_id={"ep": lax.rem(e + d, n_ep)}, device_id_type=MESH)
        return 0

    def greet_tp(d, _):
        pl.semaphore_signal(barrier, inc=1, device_id={"tp": lax.rem(t + d, n_tp)}, device_id_type=MESH)
        return 0

    lax.fori_loop(1, n_ep, greet, 0)
    lax.fori_loop(1, n_tp, greet_tp, 0)

    loads = [
        pltpu.make_async_copy(src, dst, load_sem.at[i])
        for i, (src, dst) in enumerate(
            (
                (tokens, tok_v),
                (wq, wq_v),
                (wk, wk_v),
                (wv, wv_v),
                (kc, k_v),
                (vc, v_v),
                (wo, wo_v),
                (wdg, wdg_v),
                (wdu, wdu_v),
                (weg.at[0], weg_v),
                (weu.at[0], weu_v),
                (wed.at[0], wed_v),
                (wdd, wdd_v),
            )
        )
    ]
    for load in loads:
        load.start()

    def copy_to(phase, axis, d, src, dst):
        n, me = (n_ep, e) if axis == "ep" else (n_tp, t)
        return pltpu.make_async_remote_copy(
            src_ref=src,
            dst_ref=dst,
            send_sem=send_sem.at[phase, d],
            recv_sem=recv_sem.at[phase, d],
            device_id={axis: lax.rem(me + d, n)},
            device_id_type=MESH,
        )

    def scatter(phase, axis, src, dst):
        n, me = (n_ep, e) if axis == "ep" else (n_tp, t)

        def step(d, _):
            copy_to(phase, axis, d, src.at[lax.rem(me + d, n)], dst.at[me]).start()
            return 0

        lax.fori_loop(1, n, step, 0)
        dst[me] = src[me]

    def spread(phase, axis, src, dst):
        n, me = (n_ep, e) if axis == "ep" else (n_tp, t)

        def step(d, _):
            copy_to(phase, axis, d, src, dst.at[me]).start()
            return 0

        lax.fori_loop(1, n, step, 0)
        dst[me] = src[...]

    def arrived(phase, axis, d, src, dst):
        n, me = (n_ep, e) if axis == "ep" else (n_tp, t)
        copy_to(phase, axis, d, src, dst.at[lax.rem(me - d + n, n)]).wait_recv()

    def arrive_all(phase, axis, src, dst):
        n = n_ep if axis == "ep" else n_tp

        def step(d, _):
            arrived(phase, axis, d, src, dst)
            return 0

        lax.fori_loop(1, n, step, 0)

    def sent_all(phase, axis, src, dst):
        n = n_ep if axis == "ep" else n_tp

        def step(d, _):
            copy_to(phase, axis, d, src, dst.at[0]).wait_send()
            return 0

        lax.fori_loop(1, n, step, 0)

    def total(ref, n):
        out = ref[0].astype(F32)
        for i in range(1, n):
            out = out + ref[i].astype(F32)
        return out

    loads[0].wait()
    loads[1].wait()
    tok = tok_v[...].astype(F32)
    squares = jnp.sum(tok * tok, axis=1, keepdims=True)
    scaled_in = (tok * gain[...].astype(F32)).astype(BF16)
    q_part = dot(scaled_in, wq_v[...])
    q_s[:, :, :HD] = q_part.astype(BF16).reshape(n_ep, seqs, HD)
    q_s[:, :, HD:] = hi_lo(squares, HD).astype(BF16).reshape(n_ep, seqs, HD)

    pl.semaphore_wait(barrier, n_ep + n_tp - 2)
    scatter(QP, "ep", q_s, q_r)

    loads[2].wait()
    loads[3].wait()
    kv_s[:, :, :HD] = dot(scaled_in, wk_v[...]).reshape(n_ep, seqs, HD)
    kv_s[:, :, HD:] = dot(scaled_in, wv_v[...]).reshape(n_ep, seqs, HD)
    scatter(KVP, "ep", kv_s, kv_r)

    group = rg[...].astype(F32)
    id0 = group * EPG + ri[0:1, :].astype(F32)
    id1 = group * EPG + ri[1:2, :].astype(F32)
    w0, w1 = rw[0:1, :], rw[1:2, :]
    which = lax.broadcasted_iota(jnp.int32, (n_ep, batch), 0).astype(F32)
    is0, is1 = (which == id0).astype(F32), (which == id1).astype(F32)
    before = lax.broadcasted_iota(jnp.int32, (batch, batch), 0)
    after = lax.broadcasted_iota(jnp.int32, (batch, batch), 1)
    earlier = jnp.logical_and(before < after, before // seqs == after // seqs)
    rank = dot((is0 + is1).astype(BF16), earlier.astype(F32).astype(BF16))
    block_of = (lax.broadcasted_iota(jnp.int32, (1, batch), 1) // seqs).astype(F32)
    slot0 = id0 * slots + block_of * CAP + jnp.sum(rank * is0, axis=0, keepdims=True)
    slot1 = id1 * slots + block_of * CAP + jnp.sum(rank * is1, axis=0, keepdims=True)
    slot_row = lax.broadcasted_iota(jnp.int32, (slots, batch), 0).astype(F32)
    for i in range(n_ep):
        here = slot_row + float(i * slots)
        onehot_v[i] = ((here == slot0).astype(F32) + (here == slot1).astype(F32)).astype(BF16)
    mine = slot_row + (e * slots).astype(F32)
    slot_weight = jnp.sum(
        jnp.where(mine == slot0, w0, 0.0) + jnp.where(mine == slot1, w1, 0.0), axis=1, keepdims=True
    )
    row8 = lax.broadcasted_iota(jnp.int32, (128, batch), 0)
    cols = jnp.where(row8 == 0, slot0, slot1).T
    col0, col1 = cols[:, 0:1], cols[:, 1:2]
    slot_lane = lax.broadcasted_iota(jnp.int32, (batch, width), 1).astype(F32)
    for i in range(n_ep * slots // width):
        here = slot_lane + float(i * width)
        combine_v[:, i * width : (i + 1) * width] = (
            (here == col0).astype(F32) + (here == col1).astype(F32)
        ).astype(BF16)

    arrive_all(QP, "ep", q_s.at[0], q_r)
    q_sum = total(q_r, n_ep)
    inv_first = lax.rsqrt(un_hi_lo(q_sum[:, HD:]) / depth_all + EPS)
    query = (q_sum[:, :HD] * inv_first).astype(BF16)
    loads[4].wait()
    seq_row = lax.broadcasted_iota(jnp.int32, (seqs, cache_len), 0)
    place = lax.broadcasted_iota(jnp.int32, (seqs, cache_len), 1)
    scores = jnp.zeros((seqs, cache_len), F32)
    live = jnp.zeros((seqs, cache_len), jnp.int32)
    for b in range(seqs):
        scores = jnp.where(seq_row == b, dot_nt(query, k_v[b]), scores)
        live = jnp.where(seq_row == b, lengths[b], live)
    is_live = place < live
    scores = scores / math.sqrt(HD) + shift[0]
    tail = jnp.log1p(jnp.exp(-jnp.abs(scores)))
    soft = jnp.where(is_live, jnp.maximum(scores, 0.0) + tail, 0.0)
    running = soft
    step = 1
    while step < cache_len:
        moved = pltpu.roll(running, cache_len - step, 1)
        running = running + jnp.where(place < cache_len - step, moved, 0.0)
        step *= 2
    later = running - soft
    stick = jnp.where(is_live, jnp.exp(jnp.minimum(scores, 0.0) - tail - later), 0.0).astype(BF16)
    loads[5].wait()
    out_row = lax.broadcasted_iota(jnp.int32, (seqs, HD), 0)
    attended = jnp.zeros((seqs, HD), F32)
    for b in range(seqs):
        attended = jnp.where(out_row == b, dot(stick, v_v[b]), attended)
    att_s[...] = attended.astype(BF16)
    spread(ATT, "ep", att_s, att_r)

    arrive_all(KVP, "ep", kv_s.at[0], kv_r)
    kv_sum = total(kv_r, n_ep) * inv_first
    nk_out[...] = kv_sum[:, :HD].astype(BF16)
    nv_out[...] = kv_sum[:, HD:].astype(BF16)

    loads[6].wait()
    arrive_all(ATT, "ep", att_s, att_r)
    ao_s[...] = dot(att_r[...].reshape(batch, HD), wo_v[...]).astype(BF16).reshape(n_tp, tb, width)
    scatter(AOUT, "tp", ao_s, ao_r)
    arrive_all(AOUT, "tp", ao_s.at[0], ao_r)
    own_rows = pl.ds(pl.multiple_of(t * tb, tb), tb)
    middle_own = (tok_v[own_rows, :].astype(F32) + total(ao_r, n_tp)).astype(BF16)
    mid_s[...] = middle_own
    spread(MID, "tp", mid_s, mid_r)
    arrive_all(MID, "tp", mid_s, mid_r)
    middle = mid_r[...].reshape(batch, width)

    def dispatch(d, _):
        to = lax.rem(e + d, n_ep)
        disp_s[to] = dot(onehot_v[to], middle).astype(BF16)
        copy_to(DISP, "ep", d, disp_s.at[to], disp_r.at[e]).start()
        return 0

    lax.fori_loop(1, n_ep, dispatch, 0)
    disp_r[e] = dot(onehot_v[e], middle).astype(BF16)

    mid_f = middle.astype(F32)
    mid_squares = jnp.sum(mid_f * mid_f, axis=1, keepdims=True)
    my_gain = gffn_row[:, pl.ds(pl.multiple_of(e * width, width), width)].astype(F32)
    scaled_mid = (mid_f * my_gain).astype(BF16)
    mix = jnp.sum(scaled_mid.astype(F32) * wmix[...].astype(F32), axis=1, keepdims=True)
    hidden_cols = wdg_v.shape[1]
    loads[7].wait()
    loads[8].wait()
    den_s[:, :, :hidden_cols] = dot(scaled_mid, wdg_v[...]).astype(BF16).reshape(n_ep, seqs, hidden_cols)
    den_s[:, :, hidden_cols : 2 * hidden_cols] = (
        dot(scaled_mid, wdu_v[...]).astype(BF16).reshape(n_ep, seqs, hidden_cols)
    )
    lane = lax.broadcasted_iota(jnp.int32, (batch, 128), 1)
    pair = jnp.where(lane % 2 == 0, hi_lo(mix, 128), hi_lo(mid_squares, 128))
    den_s[:, :, 2 * hidden_cols :] = pair.astype(BF16).reshape(n_ep, seqs, 128)
    scatter(DENSE, "ep", den_s, den_r)

    loads[9].wait()
    loads[10].wait()

    def expert_part(src, carry):
        gate, up, sq = carry
        rows_f = disp_r[src].astype(F32)
        at = pl.ds(pl.multiple_of(src * width, width), width)
        scaled = (rows_f * gffn_row[:, at].astype(F32)).astype(BF16)
        gate = gate + dot(scaled, weg_v[at, :])
        up = up + dot(scaled, weu_v[at, :])
        s2 = rows_f * rows_f
        for i in range(width // 128):
            sq = sq + s2[:, i * 128 : (i + 1) * 128]
        return gate, up, sq

    def expert_step(d, carry):
        arrived(DISP, "ep", d, disp_s.at[0], disp_r)
        return expert_part(lax.rem(e - d + n_ep, n_ep), carry)

    ff = weg_v.shape[1]
    zero = jnp.zeros((slots, ff), F32)
    carry = expert_part(e, (zero, zero, jnp.zeros((slots, 128), F32)))
    gate, up, sq = lax.fori_loop(1, n_ep, expert_step, carry)
    inv_rows = lax.rsqrt(jnp.sum(sq, axis=1, keepdims=True) / depth_all + EPS)
    gate = gate * inv_rows
    hidden = (gate / (1.0 + jnp.exp(-gate)) * (up * inv_rows)).astype(BF16)
    loads[11].wait()

    def give_back(d, _):
        to = lax.rem(e + d, n_ep)
        at = pl.ds(pl.multiple_of(to * width, width), width)
        ret_s[to] = (dot(hidden, wed_v[:, at]) * slot_weight).astype(BF16)
        copy_to(RET, "ep", d, ret_s.at[to], ret_r.at[e]).start()
        return 0

    lax.fori_loop(1, n_ep, give_back, 0)
    own_at = pl.ds(pl.multiple_of(e * width, width), width)
    ret_r[e] = (dot(hidden, wed_v[:, own_at]) * slot_weight).astype(BF16)

    arrive_all(DENSE, "ep", den_s.at[0], den_r)
    dense = total(den_r, n_ep)
    extra = dense[:, 2 * hidden_cols :]
    mix_sum = extra[:, 0:1] + extra[:, 64:65]
    sq_sum = extra[:, 1:2] + extra[:, 65:66]
    inv_second = lax.rsqrt(sq_sum / depth_all + EPS)
    pre = dense[:, :hidden_cols] * inv_second
    lin = dense[:, hidden_cols : 2 * hidden_cols] * inv_second
    dh_s[:, :hidden_cols] = (pre / (1.0 + jnp.exp(-pre)) * lin).astype(BF16)
    mix_gate = 1.0 / (1.0 + jnp.exp(-mix_sum * inv_second))
    dh_s[:, hidden_cols:] = hi_lo(mix_gate, 128).astype(BF16)
    spread(DHID, "ep", dh_s, dh_r)
    loads[12].wait()
    arrive_all(DHID, "ep", dh_s, dh_r)
    dh_all = dh_r[...].reshape(batch, hidden_cols + 128)
    gate_all = un_hi_lo(dh_all[:, hidden_cols:].astype(F32))
    part = dot(dh_all[:, :hidden_cols], wdd_v[...]) * gate_all

    arrive_all(RET, "ep", ret_s.at[0], ret_r)
    part = part + dot(combine_v[...], ret_r[...].reshape(n_ep * slots, width))
    fin_s[...] = part.astype(BF16).reshape(n_tp, tb, width)
    scatter(FIN, "tp", fin_s, fin_r)
    arrive_all(FIN, "tp", fin_s.at[0], fin_r)
    out_s[...] = (mid_s[...].astype(F32) + total(fin_r, n_tp)).astype(BF16)
    spread(OUT, "tp", out_s, out_r)
    arrive_all(OUT, "tp", out_s, out_r)
    mixed_out[...] = out_r[...].reshape(batch, width)

    sent_all(QP, "ep", q_s.at[0], q_r)
    sent_all(KVP, "ep", kv_s.at[0], kv_r)
    sent_all(ATT, "ep", att_s, att_r)
    sent_all(AOUT, "tp", ao_s.at[0], ao_r)
    sent_all(MID, "tp", mid_s, mid_r)
    sent_all(DISP, "ep", disp_s.at[0], disp_r)
    sent_all(DENSE, "ep", den_s.at[0], den_r)
    sent_all(DHID, "ep", dh_s, dh_r)
    sent_all(RET, "ep", ret_s.at[0], ret_r)
    sent_all(FIN, "tp", fin_s.at[0], fin_r)
    sent_all(OUT, "tp", out_s, out_r)


def on_device(n_ep, n_tp, *args):
    (
        tokens,
        gain_attn,
        w_query,
        w_key,
        w_value,
        w_output,
        key_cache,
        value_cache,
        lengths,
        score_shift,
        gain_ffn,
        w_mix,
        w_dense_gate,
        w_dense_up,
        w_dense_down,
        route_group,
        route_inner,
        route_weight,
        w_exp_gate,
        w_exp_up,
        w_exp_down,
    ) = args
    batch, width = tokens.shape
    seqs, tb = batch // n_ep, batch // n_tp
    slots = CAP * n_ep
    dense_cols = w_dense_gate.shape[1]
    n = max(n_ep, n_tp)
    anywhere = pl.BlockSpec(memory_space=pl.ANY)
    vmem = pl.BlockSpec(memory_space=pltpu.VMEM)
    smem = pl.BlockSpec(memory_space=pltpu.SMEM)

    def like(a, skip=0):
        return pltpu.VMEM(a.shape[skip:], a.dtype)

    def both(*shape, dtype=BF16):
        return [pltpu.VMEM(shape, dtype)] * 2

    return pl.pallas_call(
        functools.partial(layer, n_ep, n_tp, width * n_ep),
        out_shape=(
            jax.ShapeDtypeStruct((batch, width), BF16),
            jax.ShapeDtypeStruct((seqs, HD), BF16),
            jax.ShapeDtypeStruct((seqs, HD), BF16),
        ),
        in_specs=[
            anywhere, vmem, anywhere, anywhere, anywhere, anywhere, anywhere, anywhere,
            smem, smem, vmem, vmem, anywhere, anywhere, anywhere, vmem, vmem, vmem,
            anywhere, anywhere, anywhere,
        ],
        out_specs=(vmem, vmem, vmem),
        scratch_shapes=[
            like(tokens), like(w_query), like(w_key), like(w_value), like(w_output),
            like(key_cache), like(value_cache),
            like(w_dense_gate), like(w_dense_up), like(w_dense_down),
            like(w_exp_gate, 1), like(w_exp_up, 1), like(w_exp_down, 1),
            pltpu.VMEM((n_ep, slots, batch), BF16),
            pltpu.VMEM((batch, n_ep * slots), BF16),
            *both(n_ep, seqs, 2 * HD),
            *both(n_ep, seqs, 2 * HD, dtype=F32),
            pltpu.VMEM((seqs, HD), BF16), pltpu.VMEM((n_ep, seqs, HD), BF16),
            *both(n_tp, tb, width),
            pltpu.VMEM((tb, width), BF16), pltpu.VMEM((n_tp, tb, width), BF16),
            *both(n_ep, slots, width),
            *both(n_ep, seqs, 2 * dense_cols + 128),
            pltpu.VMEM((seqs, dense_cols + 128), BF16),
            pltpu.VMEM((n_ep, seqs, dense_cols + 128), BF16),
            *both(n_ep, slots, width),
            *both(n_tp, tb, width),
            pltpu.VMEM((tb, width), BF16), pltpu.VMEM((n_tp, tb, width), BF16),
            pltpu.SemaphoreType.DMA((13,)),
            pltpu.SemaphoreType.DMA((N_PHASE, n)),
            pltpu.SemaphoreType.DMA((N_PHASE, n)),
        ],
        compiler_params=pltpu.CompilerParams(
            collective_id=0, has_side_effects=True, vmem_limit_bytes=VMEM_BYTES
        ),
        name="decode_layer",
    )(
        tokens, gain_attn[None, :], w_query, w_key, w_value, w_output, key_cache, value_cache,
        lengths, score_shift, gain_ffn[None, :], w_mix[None, :],
        w_dense_gate, w_dense_up, w_dense_down,
        route_group[None, :], route_inner.T, route_weight.T,
        w_exp_gate, w_exp_up, w_exp_down,
    )


def solution(mesh):
    placed = (
        P(None, "ep"),
        P("ep"),
        P("ep", "tp"),
        P("ep", "tp"),
        P("ep", "tp"),
        P("tp", "ep"),
        P("ep", None, "tp"),
        P("ep", None, "tp"),
        P("ep"),
        P("tp"),
        P(),
        P("ep"),
        P("ep", "tp"),
        P("ep", "tp"),
        P("tp", "ep"),
        P(),
        P(),
        P(),
        P("ep", None, "tp"),
        P("ep", None, "tp"),
        P("ep", "tp", None),
    )
    return jax.shard_map(
        functools.partial(on_device, mesh.shape["ep"], mesh.shape["tp"]),
        mesh=mesh,
        in_specs=placed,
        out_specs=(P(None, "ep"), P("ep", "tp"), P("ep", "tp")),
        check_vma=False,
    )
```

```python
import functools
import math

import jax
import jax.numpy as jnp
from jax import lax
from jax.experimental import pallas as pl
from jax.experimental.pallas import tpu as pltpu
from jax.sharding import PartitionSpec as P

MESH = pl.DeviceIdType.MESH
HD = 128
EPG = 4
CAP = 4
EPS = 1e-06
F32 = jnp.float32
BF16 = jnp.bfloat16

QP, KVP, ATT, AOUT, MID, DISP, DENSE, DHID, RET, FIN, OUT = range(11)
N_PHASE = 11
WDOWN, HID, DPART, N_PAIR = 15, 16, 17, 18
VMEM_BYTES = 67_043_328 - 0 * 1024


def dot(a, b):
    return jnp.dot(a, b, preferred_element_type=F32)


def dot_nt(a, b):
    return lax.dot_general(a, b, (((1,), (1,)), ((), ())), preferred_element_type=F32)


def hi_lo(col, width):
    rows = col.shape[0]
    hi = col.astype(BF16).astype(F32)
    lane = lax.broadcasted_iota(jnp.int32, (rows, width), 1)
    return jnp.where(lane < width // 2, hi, col - hi)


def un_hi_lo(pair):
    half = pair.shape[1] // 2
    return pair[:, 0:1] + pair[:, half : half + 1]


def ring(d, n):
    return min(d % n, n - d % n)


def offsets_ep(n):
    if n != 16:
        return [(0, d) for d in range(1, n)], n
    pairs = [(a, b) for a in range(4) for b in range(4) if a or b]
    return sorted(pairs, key=lambda p: -ring(p[0], 4) - ring(p[1], 4)), 4


def offsets_tp(n):
    pairs = [(a, b) for a in range(n // 2) for b in range(2) if a or b]
    return sorted(pairs, key=lambda p: -ring(p[0], n // 2) * 2 - p[1]), 2


def partners(me, offsets, minor, n):
    major = n // minor
    hi, lo = me // minor, lax.rem(me, minor)
    to = [lax.rem(hi + a, major) * minor + lax.rem(lo + b, minor) for a, b in offsets]
    back = [lax.rem(hi - a + major, major) * minor + lax.rem(lo - b + minor, minor) for a, b in offsets]
    return to, back


def layer(
    n_ep,
    n_tp,
    depth_all,
    tokens,
    gain,
    wq,
    wk,
    wv,
    wo,
    kc,
    vc,
    lengths,
    shift,
    gffn,
    wmix,
    wdg,
    wdu,
    wdd,
    rg,
    ri,
    rw,
    weg,
    weu,
    wed,
    mixed_out,
    nk_out,
    nv_out,
    tok_v,
    wq_v,
    wk_v,
    wv_v,
    wo_v,
    k_v,
    v_v,
    wdg_v,
    wdu_v,
    wdd_v,
    wgu_v,
    wed_v,
    wed_o,
    gain_v,
    len_v,
    shift_v,
    gffn_v,
    wmix_v,
    rg_v,
    ri_v,
    rw_v,
    gffn_row,
    onehot_v,
    combine_v,
    q_s,
    q_r,
    kv_s,
    kv_r,
    att_s,
    att_r,
    ao_s,
    ao_r,
    mid_s,
    mid_r,
    disp_s,
    disp_r,
    disp_o,
    den_s,
    den_r,
    dh_s,
    dh_r,
    hid_s,
    hid_r,
    ret_s,
    ret_r,
    dp_s,
    dp_r,
    fin_s,
    fin_r,
    out_s,
    out_r,
    load_sem,
    send_sem,
    recv_sem,
    pair_send,
    pair_recv,
):
    e = lax.axis_index("ep")
    t = lax.axis_index("tp")
    batch, width = tok_v.shape
    seqs = batch // n_ep
    tb = batch // n_tp
    slots = CAP * n_ep
    cache_len = k_v.shape[1]
    ff = wgu_v.shape[1] // 2

    ep_to, ep_from = partners(e, *offsets_ep(n_ep), n_ep)
    tp_to, tp_from = partners(t, *offsets_tp(n_tp), n_tp)
    z, core = t // 2, lax.rem(t, 2)
    n_z = n_tp // 2
    far_z = sorted(range(1, n_z), key=lambda a: -ring(a, n_z))
    z_to = [lax.rem(z + a, n_z) for a in far_z]
    z_from = [lax.rem(z - a + n_z, n_z) for a in far_z]
    to_of = {"ep": ep_to, "tp": tp_to, "z": z_to}
    from_of = {"ep": ep_from, "tp": tp_from, "z": z_from}
    me_of = {"ep": e, "tp": t, "z": z}
    half = width // 2
    own_half = pl.ds(pl.multiple_of(core * half, half), half)
    other_half = pl.ds(pl.multiple_of((1 - core) * half, half), half)

    barrier = pltpu.get_barrier_semaphore()
    for axis in ("ep", "tp"):
        for peer in to_of[axis]:
            pl.semaphore_signal(barrier, inc=1, device_id={axis: peer}, device_id_type=MESH)

    loads = [
        pltpu.make_async_copy(src, dst, load_sem.at[i])
        for i, (src, dst) in enumerate(
            (
                (tokens, tok_v),
                (wq, wq_v),
                (wk, wk_v),
                (wv, wv_v),
                (kc, k_v),
                (vc, v_v),
                (wo, wo_v),
                (wdg, wdg_v),
                (wdu, wdu_v),
                (weg.at[0], wgu_v.at[:, :ff]),
                (weu.at[0], wgu_v.at[:, ff:]),
                (wed.at[0], wed_v),
                (wdd, wdd_v),
                (gain, gain_v),
                (lengths, len_v),
                (shift, shift_v),
                (gffn, gffn_v),
                (wmix, wmix_v),
                (rg, rg_v),
                (ri, ri_v),
                (rw, rw_v),
            )
        )
    ]
    for load in loads:
        load.start()

    def copy_to(phase, axis, k, src, dst):
        return pltpu.make_async_remote_copy(
            src_ref=src,
            dst_ref=dst,
            send_sem=send_sem.at[phase, k],
            recv_sem=recv_sem.at[phase, k],
            device_id={"tp": to_of[axis][k] * 2 + core} if axis == "z" else {axis: to_of[axis][k]},
            device_id_type=MESH,
        )

    def to_partner(k, src, dst):
        return pltpu.make_async_remote_copy(
            src_ref=src,
            dst_ref=dst,
            send_sem=pair_send.at[k],
            recv_sem=pair_recv.at[k],
            device_id={"tp": 2 * z + 1 - core},
            device_id_type=MESH,
        )

    def scatter(phase, axis, src, dst):
        me = me_of[axis]
        for k, to in enumerate(to_of[axis]):
            copy_to(phase, axis, k, src.at[to], dst.at[me]).start()
        dst[me] = src[me]

    def spread(phase, axis, src, dst):
        me = me_of[axis]
        for k in range(len(to_of[axis])):
            copy_to(phase, axis, k, src, dst.at[me]).start()
        dst[me] = src[...]

    def arrived(phase, axis, k, src, dst):
        copy_to(phase, axis, k, src, dst.at[from_of[axis][k]]).wait_recv()

    def arrive_all(phase, axis, src, dst):
        for k in range(len(to_of[axis])):
            arrived(phase, axis, k, src, dst)

    def sent_all(phase, axis, src, dst):
        for k in range(len(to_of[axis])):
            copy_to(phase, axis, k, src, dst.at[0]).wait_send()

    def total(ref, n):
        out = ref[0].astype(F32)
        for i in range(1, n):
            out = out + ref[i].astype(F32)
        return out

    loads[0].wait()
    loads[1].wait()
    loads[13].wait()
    tok = tok_v[...].astype(F32)
    squares = jnp.sum(tok * tok, axis=1, keepdims=True)
    scaled_in = (tok * gain_v[...].astype(F32)[None, :]).astype(BF16)
    q_part = dot(scaled_in, wq_v[...])
    q_s[:, :, :HD] = q_part.astype(BF16).reshape(n_ep, seqs, HD)
    q_s[:, :, HD:] = hi_lo(squares, HD).astype(BF16).reshape(n_ep, seqs, HD)

    pl.semaphore_wait(barrier, n_ep + n_tp - 2)
    scatter(QP, "ep", q_s, q_r)

    loads[2].wait()
    loads[3].wait()
    kv_s[:, :, :HD] = dot(scaled_in, wk_v[...]).reshape(n_ep, seqs, HD)
    kv_s[:, :, HD:] = dot(scaled_in, wv_v[...]).reshape(n_ep, seqs, HD)

    for i in range(14, 21):
        loads[i].wait()
    gffn_row[...] = gffn_v[...].astype(F32)[None, :]
    group = rg_v[...].astype(F32)[None, :]
    id0 = group * EPG + ri_v[0:1, :].astype(F32)
    id1 = group * EPG + ri_v[1:2, :].astype(F32)
    w0, w1 = rw_v[0:1, :], rw_v[1:2, :]
    which = lax.broadcasted_iota(jnp.int32, (n_ep, batch), 0).astype(F32)
    is0, is1 = (which == id0).astype(F32), (which == id1).astype(F32)
    before = lax.broadcasted_iota(jnp.int32, (batch, batch), 0)
    after = lax.broadcasted_iota(jnp.int32, (batch, batch), 1)
    earlier = jnp.logical_and(before < after, before // seqs == after // seqs)
    rank = dot((is0 + is1).astype(BF16), earlier.astype(F32).astype(BF16))
    block_of = (lax.broadcasted_iota(jnp.int32, (1, batch), 1) // seqs).astype(F32)
    slot0 = id0 * slots + block_of * CAP + jnp.sum(rank * is0, axis=0, keepdims=True)
    slot1 = id1 * slots + block_of * CAP + jnp.sum(rank * is1, axis=0, keepdims=True)
    slot_row = lax.broadcasted_iota(jnp.int32, (slots, batch), 0).astype(F32)
    for i in range(n_ep):
        here = slot_row + float(i * slots)
        onehot_v[i] = ((here == slot0).astype(F32) + (here == slot1).astype(F32)).astype(BF16)
    mine = slot_row + (e * slots).astype(F32)
    slot_weight = jnp.sum(
        jnp.where(mine == slot0, w0, 0.0) + jnp.where(mine == slot1, w1, 0.0), axis=1, keepdims=True
    )
    row8 = lax.broadcasted_iota(jnp.int32, (128, batch), 0)
    cols = jnp.where(row8 == 0, slot0, slot1).T
    col0, col1 = cols[:, 0:1], cols[:, 1:2]
    slot_lane = lax.broadcasted_iota(jnp.int32, (batch, width), 1).astype(F32)
    for i in range(n_ep * slots // width):
        here = slot_lane + float(i * width)
        combine_v[:, i * width : (i + 1) * width] = (
            (here == col0).astype(F32) + (here == col1).astype(F32)
        ).astype(BF16)

    loads[11].wait()
    for i in range(n_ep):
        at = pl.ds(pl.multiple_of(i * width + (1 - core) * half, half), half)
        to_partner(WDOWN, wed_v.at[:, at], wed_o.at[:, i * half : (i + 1) * half]).start()

    arrive_all(QP, "ep", q_s.at[0], q_r)
    q_sum = total(q_r, n_ep)
    inv_first = lax.rsqrt(un_hi_lo(q_sum[:, HD:]) / depth_all + EPS)
    query = (q_sum[:, :HD] * inv_first).astype(BF16)
    loads[4].wait()
    seq_row = lax.broadcasted_iota(jnp.int32, (seqs, cache_len), 0)
    place = lax.broadcasted_iota(jnp.int32, (seqs, cache_len), 1)
    scores = jnp.zeros((seqs, cache_len), F32)
    live = jnp.zeros((seqs, cache_len), jnp.int32)
    for b in range(seqs):
        scores = jnp.where(seq_row == b, dot_nt(query, k_v[b]), scores)
        live = jnp.where(seq_row == b, len_v[b], live)
    is_live = place < live
    scores = scores / math.sqrt(HD) + shift_v[0]
    tail = jnp.log1p(jnp.exp(-jnp.abs(scores)))
    soft = jnp.where(is_live, jnp.maximum(scores, 0.0) + tail, 0.0)
    running = soft
    step = 1
    while step < cache_len:
        moved = pltpu.roll(running, cache_len - step, 1)
        running = running + jnp.where(place < cache_len - step, moved, 0.0)
        step *= 2
    later = running - soft
    stick = jnp.where(is_live, jnp.exp(jnp.minimum(scores, 0.0) - tail - later), 0.0).astype(BF16)
    loads[5].wait()
    out_row = lax.broadcasted_iota(jnp.int32, (seqs, HD), 0)
    attended = jnp.zeros((seqs, HD), F32)
    for b in range(seqs):
        attended = jnp.where(out_row == b, dot(stick, v_v[b]), attended)
    att_s[...] = attended.astype(BF16)
    spread(ATT, "ep", att_s, att_r)

    loads[6].wait()
    arrive_all(ATT, "ep", att_s, att_r)
    ao_s[...] = dot(att_r[...].reshape(batch, HD), wo_v[...]).astype(BF16).reshape(n_tp, tb, width)
    scatter(AOUT, "tp", ao_s, ao_r)
    scatter(KVP, "ep", kv_s, kv_r)
    arrive_all(AOUT, "tp", ao_s.at[0], ao_r)
    own_rows = pl.ds(pl.multiple_of(t * tb, tb), tb)
    middle_own = (tok_v[own_rows, :].astype(F32) + total(ao_r, n_tp)).astype(BF16)
    mid_s[...] = middle_own
    spread(MID, "tp", mid_s, mid_r)

    arrive_all(KVP, "ep", kv_s.at[0], kv_r)
    kv_sum = total(kv_r, n_ep) * inv_first
    nk_out[...] = kv_sum[:, :HD].astype(BF16)
    nv_out[...] = kv_sum[:, HD:].astype(BF16)

    arrive_all(MID, "tp", mid_s, mid_r)
    middle = mid_r[...].reshape(batch, width)

    mid_own = mid_r[:, :, own_half].reshape(batch, half)
    mid_other = mid_r[:, :, other_half].reshape(batch, half)
    for k, to in enumerate(ep_to):
        disp_s[to] = dot(onehot_v[to], mid_own).astype(BF16)
        copy_to(DISP, "ep", k, disp_s.at[to], disp_r.at[e]).start()
    disp_r[e] = dot(onehot_v[e], mid_own).astype(BF16)
    disp_o[e] = dot(onehot_v[e], mid_other).astype(BF16)

    mid_f = middle.astype(F32)
    mid_squares = jnp.sum(mid_f * mid_f, axis=1, keepdims=True)
    my_gain = gffn_row[:, pl.ds(pl.multiple_of(e * width, width), width)]
    scaled_mid = (mid_f * my_gain).astype(BF16)
    mix = jnp.sum(scaled_mid.astype(F32) * wmix_v[...].astype(F32)[None, :], axis=1, keepdims=True)
    hidden_cols = wdg_v.shape[1]
    loads[7].wait()
    loads[8].wait()
    den_s[:, :, :hidden_cols] = dot(scaled_mid, wdg_v[...]).astype(BF16).reshape(n_ep, seqs, hidden_cols)
    den_s[:, :, hidden_cols : 2 * hidden_cols] = (
        dot(scaled_mid, wdu_v[...]).astype(BF16).reshape(n_ep, seqs, hidden_cols)
    )
    lane = lax.broadcasted_iota(jnp.int32, (batch, 128), 1)
    pair = jnp.where(lane % 2 == 0, hi_lo(mix, 128), hi_lo(mid_squares, 128))
    den_s[:, :, 2 * hidden_cols :] = pair.astype(BF16).reshape(n_ep, seqs, 128)
    scatter(DENSE, "ep", den_s, den_r)

    loads[9].wait()
    loads[10].wait()

    def expert_part(ref, src, part, carry):
        acc, sq = carry
        rows_f = ref[src].astype(F32)
        at = pl.ds(pl.multiple_of(src * width + part * half, half), half)
        scaled = (rows_f * gffn_row[:, at]).astype(BF16)
        return acc + dot(scaled, wgu_v[at, :]), sq + rows_f * rows_f

    carry = (jnp.zeros((slots, 2 * ff), F32), jnp.zeros((slots, half), F32))
    carry = expert_part(disp_r, e, core, carry)
    carry = expert_part(disp_o, e, 1 - core, carry)
    nearest_first = list(reversed(range(n_ep - 1)))
    for k in nearest_first:
        arrived(DISP, "ep", k, disp_s.at[0], disp_r)
        to_partner(k, disp_r.at[ep_from[k]], disp_o.at[ep_from[k]]).start()
        carry = expert_part(disp_r, ep_from[k], core, carry)
    for k in nearest_first:
        to_partner(k, disp_r.at[ep_from[k]], disp_o.at[ep_from[k]]).wait_recv()
        carry = expert_part(disp_o, ep_from[k], 1 - core, carry)
    acc, sq = carry
    inv_rows = lax.rsqrt(jnp.sum(sq, axis=1, keepdims=True) / depth_all + EPS)
    gate = acc[:, :ff] * inv_rows
    hid_s[...] = (gate / (1.0 + jnp.exp(-gate)) * (acc[:, ff:] * inv_rows)).astype(BF16)
    to_partner(HID, hid_s, hid_r).start()
    to_partner(WDOWN, wed_o, wed_o).wait_recv()
    to_partner(HID, hid_s, hid_r).wait_recv()
    hidden, hidden_o = hid_s[...], hid_r[...]

    def down(to):
        at = pl.ds(pl.multiple_of(to * width + core * half, half), half)
        at_o = pl.ds(pl.multiple_of(to * half, half), half)
        return ((dot(hidden, wed_v[:, at]) + dot(hidden_o, wed_o[:, at_o])) * slot_weight).astype(BF16)

    for k, to in enumerate(ep_to):
        ret_s[to] = down(to)
        copy_to(RET, "ep", k, ret_s.at[to], ret_r.at[e]).start()
    ret_r[e] = down(e)

    arrive_all(DENSE, "ep", den_s.at[0], den_r)
    dense = total(den_r, n_ep)
    extra = dense[:, 2 * hidden_cols :]
    mix_sum = extra[:, 0:1] + extra[:, 64:65]
    sq_sum = extra[:, 1:2] + extra[:, 65:66]
    inv_second = lax.rsqrt(sq_sum / depth_all + EPS)
    pre = dense[:, :hidden_cols] * inv_second
    lin = dense[:, hidden_cols : 2 * hidden_cols] * inv_second
    dh_s[:, :hidden_cols] = (pre / (1.0 + jnp.exp(-pre)) * lin).astype(BF16)
    mix_gate = 1.0 / (1.0 + jnp.exp(-mix_sum * inv_second))
    dh_s[:, hidden_cols:] = hi_lo(mix_gate, 128).astype(BF16)
    spread(DHID, "ep", dh_s, dh_r)
    loads[12].wait()
    arrive_all(DHID, "ep", dh_s, dh_r)
    dh_all = dh_r[...].reshape(batch, hidden_cols + 128)
    gate_all = un_hi_lo(dh_all[:, hidden_cols:].astype(F32))
    dense_in = dh_all[:, :hidden_cols]
    dp_s[...] = dot(dense_in, wdd_v[:, other_half]) * gate_all
    to_partner(DPART, dp_s, dp_r).start()
    part = dot(dense_in, wdd_v[:, own_half]) * gate_all

    arrive_all(RET, "ep", ret_s.at[0], ret_r)
    part = part + dot(combine_v[...], ret_r[...].reshape(n_ep * slots, half))
    to_partner(DPART, dp_s, dp_r).wait_recv()
    fin_s[...] = (part + dp_r[...]).astype(BF16).reshape(n_z, 2 * tb, half)
    scatter(FIN, "z", fin_s, fin_r)
    arrive_all(FIN, "z", fin_s.at[0], fin_r)
    mid_here = mid_r[pl.ds(2 * z, 2), :, own_half].reshape(2 * tb, half)
    out_s[...] = (mid_here.astype(F32) + total(fin_r, n_z)).astype(BF16)
    spread(OUT, "tp", out_s, out_r)
    arrive_all(OUT, "tp", out_s, out_r)
    for i in range(n_tp):
        at = slice(i // 2 * 2 * tb, (i // 2 + 1) * 2 * tb)
        mixed_out[at, i % 2 * half : (i % 2 + 1) * half] = out_r[i]

    sent_all(QP, "ep", q_s.at[0], q_r)
    sent_all(KVP, "ep", kv_s.at[0], kv_r)
    sent_all(ATT, "ep", att_s, att_r)
    sent_all(AOUT, "tp", ao_s.at[0], ao_r)
    sent_all(MID, "tp", mid_s, mid_r)
    sent_all(DISP, "ep", disp_s.at[0], disp_r)
    sent_all(DENSE, "ep", den_s.at[0], den_r)
    sent_all(DHID, "ep", dh_s, dh_r)
    sent_all(RET, "ep", ret_s.at[0], ret_r)
    sent_all(FIN, "z", fin_s.at[0], fin_r)
    sent_all(OUT, "tp", out_s, out_r)
    for k in range(n_ep - 1):
        to_partner(k, disp_r.at[0], disp_o.at[0]).wait_send()
    to_partner(WDOWN, wed_o, wed_o).wait_send()
    to_partner(HID, hid_s, hid_r).wait_send()
    to_partner(DPART, dp_s, dp_r).wait_send()


def write_out(mixed, keys, values, mixed_out, keys_out, values_out, sem):
    pairs = ((mixed, mixed_out), (keys, keys_out), (values, values_out))
    copies = [pltpu.make_async_copy(a, b, sem.at[i]) for i, (a, b) in enumerate(pairs)]
    for copy in copies:
        copy.start()
    for copy in copies:
        copy.wait()


def on_device(n_ep, n_tp, *args):
    (
        tokens,
        gain_attn,
        w_query,
        w_key,
        w_value,
        w_output,
        key_cache,
        value_cache,
        lengths,
        score_shift,
        gain_ffn,
        w_mix,
        w_dense_gate,
        w_dense_up,
        w_dense_down,
        route_group,
        route_inner,
        route_weight,
        w_exp_gate,
        w_exp_up,
        w_exp_down,
    ) = args
    batch, width = tokens.shape
    seqs, tb = batch // n_ep, batch // n_tp
    slots, half = CAP * n_ep, width // 2
    dense_cols = w_dense_gate.shape[1]
    n = max(n_ep, n_tp)
    vmem = pl.BlockSpec(memory_space=pltpu.VMEM)
    hbm = pl.BlockSpec(memory_space=pltpu.HBM)

    def like(a, skip=0):
        return pltpu.VMEM(a.shape[skip:], a.dtype)

    def both(*shape, dtype=BF16):
        return [pltpu.VMEM(shape, dtype)] * 2

    results = pl.pallas_call(
        functools.partial(layer, n_ep, n_tp, width * n_ep),
        out_shape=(
            jax.ShapeDtypeStruct((batch, width), BF16),
            jax.ShapeDtypeStruct((seqs, HD), BF16),
            jax.ShapeDtypeStruct((seqs, HD), BF16),
        ),
        in_specs=[hbm] * 21,
        out_specs=(vmem, vmem, vmem),
        scratch_shapes=[
            like(tokens), like(w_query), like(w_key), like(w_value), like(w_output),
            like(key_cache), like(value_cache),
            like(w_dense_gate), like(w_dense_up), like(w_dense_down),
            pltpu.VMEM((w_exp_gate.shape[1], 2 * w_exp_gate.shape[2]), BF16), like(w_exp_down, 1),
            pltpu.VMEM((w_exp_down.shape[1], w_exp_down.shape[2] // 2), BF16),
            like(gain_attn), pltpu.SMEM(lengths.shape, lengths.dtype),
            pltpu.SMEM(score_shift.shape, score_shift.dtype), like(gain_ffn), like(w_mix),
            like(route_group), like(route_inner.T), like(route_weight.T),
            pltpu.VMEM((1, gain_ffn.shape[0]), F32),
            pltpu.VMEM((n_ep, slots, batch), BF16),
            pltpu.VMEM((batch, n_ep * slots), BF16),
            *both(n_ep, seqs, 2 * HD),
            *both(n_ep, seqs, 2 * HD, dtype=F32),
            pltpu.VMEM((seqs, HD), BF16), pltpu.VMEM((n_ep, seqs, HD), BF16),
            *both(n_tp, tb, width),
            pltpu.VMEM((tb, width), BF16), pltpu.VMEM((n_tp, tb, width), BF16),
            *both(n_ep, slots, half), pltpu.VMEM((n_ep, slots, half), BF16),
            *both(n_ep, seqs, 2 * dense_cols + 128),
            pltpu.VMEM((seqs, dense_cols + 128), BF16),
            pltpu.VMEM((n_ep, seqs, dense_cols + 128), BF16),
            *both(slots, w_exp_gate.shape[2]),
            *both(n_ep, slots, half),
            *both(batch, half, dtype=F32),
            *both(n_tp // 2, 2 * tb, half),
            pltpu.VMEM((2 * tb, half), BF16), pltpu.VMEM((n_tp, 2 * tb, half), BF16),
            pltpu.SemaphoreType.DMA((21,)),
            pltpu.SemaphoreType.DMA((N_PHASE, n)),
            pltpu.SemaphoreType.DMA((N_PHASE, n)),
            pltpu.SemaphoreType.DMA((N_PAIR,)),
            pltpu.SemaphoreType.DMA((N_PAIR,)),
        ],
        compiler_params=pltpu.CompilerParams(
            collective_id=0, has_side_effects=True, vmem_limit_bytes=VMEM_BYTES
        ),
        name="decode_layer",
    )(
        tokens, gain_attn, w_query, w_key, w_value, w_output, key_cache, value_cache,
        lengths, score_shift, gain_ffn, w_mix,
        w_dense_gate, w_dense_up, w_dense_down,
        route_group, route_inner.T, route_weight.T,
        w_exp_gate, w_exp_up, w_exp_down,
    )
    return pl.pallas_call(
        write_out,
        out_shape=tuple(jax.ShapeDtypeStruct(r.shape, r.dtype) for r in results),
        in_specs=[vmem] * 3,
        out_specs=(hbm, hbm, hbm),
        scratch_shapes=[pltpu.SemaphoreType.DMA((3,))],
        compiler_params=pltpu.CompilerParams(vmem_limit_bytes=1024 * 1024),
        name="write_out",
    )(*results)


def solution(mesh):
    placed = (
        P(None, "ep"),
        P("ep"),
        P("ep", "tp"),
        P("ep", "tp"),
        P("ep", "tp"),
        P("tp", "ep"),
        P("ep", None, "tp"),
        P("ep", None, "tp"),
        P("ep"),
        P("tp"),
        P(),
        P("ep"),
        P("ep", "tp"),
        P("ep", "tp"),
        P("tp", "ep"),
        P(),
        P(),
        P(),
        P("ep", None, "tp"),
        P("ep", None, "tp"),
        P("ep", "tp", None),
    )
    return jax.shard_map(
        functools.partial(on_device, mesh.shape["ep"], mesh.shape["tp"]),
        mesh=mesh,
        in_specs=placed,
        out_specs=(P(None, "ep"), P("ep", "tp"), P("ep", "tp")),
        check_vma=False,
    )
```

```python
import functools
import math

import jax
import jax.numpy as jnp
from jax import lax
from jax.experimental import pallas as pl
from jax.experimental.pallas import tpu as pltpu
from jax.sharding import PartitionSpec as P

MESH = pl.DeviceIdType.MESH
HD = 128
EPG = 4
CAP = 4
EPS = 1e-06
F32 = jnp.float32
BF16 = jnp.bfloat16

QP, KVP, ATT, AOUT, MID, DISP, DENSE, DHID, RET, FIN, OUT = range(11)
N_PHASE = 11
WDOWN, HID, DPART, N_PAIR = 15, 16, 17, 18
VMEM_BYTES = 67_043_328 - 0 * 1024


def dot(a, b):
    return jnp.dot(a, b, preferred_element_type=F32)


def dot_nt(a, b):
    return lax.dot_general(a, b, (((1,), (1,)), ((), ())), preferred_element_type=F32)


def hi_lo(col, width):
    rows = col.shape[0]
    hi = col.astype(BF16).astype(F32)
    lane = lax.broadcasted_iota(jnp.int32, (rows, width), 1)
    return jnp.where(lane < width // 2, hi, col - hi)


def un_hi_lo(pair):
    half = pair.shape[1] // 2
    return pair[:, 0:1] + pair[:, half : half + 1]


def ring(d, n):
    return min(d % n, n - d % n)


def offsets_ep(n):
    if n != 16:
        return [(0, d) for d in range(1, n)], n
    pairs = [(a, b) for a in range(4) for b in range(4) if a or b]
    return sorted(pairs, key=lambda p: -ring(p[0], 4) - ring(p[1], 4)), 4


def offsets_tp(n):
    pairs = [(a, b) for a in range(n // 2) for b in range(2) if a or b]
    return sorted(pairs, key=lambda p: -ring(p[0], n // 2) * 2 - p[1]), 2


def partners(me, offsets, minor, n):
    major = n // minor
    hi, lo = me // minor, lax.rem(me, minor)
    to = [lax.rem(hi + a, major) * minor + lax.rem(lo + b, minor) for a, b in offsets]
    back = [lax.rem(hi - a + major, major) * minor + lax.rem(lo - b + minor, minor) for a, b in offsets]
    return to, back


def layer(
    n_ep,
    n_tp,
    depth_all,
    tokens,
    gain,
    wq,
    wk,
    wv,
    wo,
    kc,
    vc,
    lengths,
    shift,
    gffn,
    wmix,
    wdg,
    wdu,
    wdd,
    rg,
    ri,
    rw,
    weg,
    weu,
    wed,
    mixed_out,
    nk_out,
    nv_out,
    tok_v,
    wq_v,
    wk_v,
    wv_v,
    wo_v,
    k_v,
    v_v,
    wdg_v,
    wdu_v,
    wdd_v,
    wgu_v,
    wdn_v,
    gain_v,
    len_v,
    shift_v,
    gffn_v,
    wmix_v,
    rg_v,
    ri_v,
    rw_v,
    gffn_row,
    onehot_v,
    combine_v,
    q_s,
    q_r,
    kv_s,
    kv_r,
    att_s,
    att_r,
    ao_s,
    ao_r,
    mid_s,
    mid_r,
    disp_s,
    disp_r,
    disp_o,
    den_s,
    den_r,
    dh_s,
    dh_r,
    hid_s,
    hid_r,
    ret_s,
    ret_r,
    dp_s,
    dp_r,
    fin_s,
    fin_r,
    out_s,
    out_r,
    load_sem,
    down_sem,
    send_sem,
    recv_sem,
    pair_send,
    pair_recv,
):
    e = lax.axis_index("ep")
    t = lax.axis_index("tp")
    batch, width = tok_v.shape
    seqs = batch // n_ep
    tb = batch // n_tp
    slots = CAP * n_ep
    cache_len = k_v.shape[1]
    ff = wgu_v.shape[1] // 2

    ep_to, ep_from = partners(e, *offsets_ep(n_ep), n_ep)
    tp_to, tp_from = partners(t, *offsets_tp(n_tp), n_tp)
    z, core = t // 2, lax.rem(t, 2)
    n_z = n_tp // 2
    far_z = sorted(range(1, n_z), key=lambda a: -ring(a, n_z))
    z_to = [lax.rem(z + a, n_z) for a in far_z]
    z_from = [lax.rem(z - a + n_z, n_z) for a in far_z]
    to_of = {"ep": ep_to, "tp": tp_to, "z": z_to}
    from_of = {"ep": ep_from, "tp": tp_from, "z": z_from}
    me_of = {"ep": e, "tp": t, "z": z}
    half = width // 2
    own_half = pl.ds(pl.multiple_of(core * half, half), half)
    other_half = pl.ds(pl.multiple_of((1 - core) * half, half), half)

    barrier = pltpu.get_barrier_semaphore()
    for axis in ("ep", "tp"):
        for peer in to_of[axis]:
            pl.semaphore_signal(barrier, inc=1, device_id={axis: peer}, device_id_type=MESH)

    loads = [
        pltpu.make_async_copy(src, dst, load_sem.at[i])
        for i, (src, dst) in enumerate(
            (
                (tokens, tok_v),
                (wq, wq_v),
                (wk, wk_v),
                (wv, wv_v),
                (kc, k_v),
                (vc, v_v),
                (wo, wo_v),
                (wdg, wdg_v),
                (wdu, wdu_v),
                (weg.at[0], wgu_v.at[:, :ff]),
                (weu.at[0], wgu_v.at[:, ff:]),
                (wmix, wmix_v),
                (wdd, wdd_v),
                (gain, gain_v),
                (lengths, len_v),
                (shift, shift_v),
                (gffn, gffn_v),
                (rg, rg_v),
                (ri, ri_v),
                (rw, rw_v),
            )
        )
    ]
    for i in (0, 1, 13, 2, 3, 17, 18, 19, 16, 14, 15, 11, 4, 5, 6, 7, 8, 9, 10, 12):
        loads[i].start()
    for i in range(n_ep):
        at = pl.ds(pl.multiple_of(i * width + core * half, half), half)
        pltpu.make_async_copy(wed.at[0, :, at], wdn_v.at[:ff, i * half : (i + 1) * half], down_sem).start()

    def copy_to(phase, axis, k, src, dst):
        return pltpu.make_async_remote_copy(
            src_ref=src,
            dst_ref=dst,
            send_sem=send_sem.at[phase, k],
            recv_sem=recv_sem.at[phase, k],
            device_id={"tp": to_of[axis][k] * 2 + core} if axis == "z" else {axis: to_of[axis][k]},
            device_id_type=MESH,
        )

    def to_partner(k, src, dst):
        return pltpu.make_async_remote_copy(
            src_ref=src,
            dst_ref=dst,
            send_sem=pair_send.at[k],
            recv_sem=pair_recv.at[k],
            device_id={"tp": 2 * z + 1 - core},
            device_id_type=MESH,
        )

    def scatter(phase, axis, src, dst):
        me = me_of[axis]
        for k, to in enumerate(to_of[axis]):
            copy_to(phase, axis, k, src.at[to], dst.at[me]).start()
        dst[me] = src[me]

    def spread(phase, axis, src, dst):
        me = me_of[axis]
        for k in range(len(to_of[axis])):
            copy_to(phase, axis, k, src, dst.at[me]).start()
        dst[me] = src[...]

    def arrived(phase, axis, k, src, dst):
        copy_to(phase, axis, k, src, dst.at[from_of[axis][k]]).wait_recv()

    def arrive_all(phase, axis, src, dst):
        for k in range(len(to_of[axis])):
            arrived(phase, axis, k, src, dst)

    def sent_all(phase, axis, src, dst):
        for k in range(len(to_of[axis])):
            copy_to(phase, axis, k, src, dst.at[0]).wait_send()

    def total(ref, n):
        out = ref[0].astype(F32)
        for i in range(1, n):
            out = out + ref[i].astype(F32)
        return out

    loads[0].wait()
    loads[1].wait()
    loads[13].wait()
    tok = tok_v[...].astype(F32)
    squares = jnp.sum(tok * tok, axis=1, keepdims=True)
    scaled_in = (tok * gain_v[...].astype(F32)[None, :]).astype(BF16)
    q_part = dot(scaled_in, wq_v[...])
    q_s[:, :, :HD] = q_part.astype(BF16).reshape(n_ep, seqs, HD)
    q_s[:, :, HD:] = hi_lo(squares, HD).astype(BF16).reshape(n_ep, seqs, HD)

    pl.semaphore_wait(barrier, n_ep + n_tp - 2)
    scatter(QP, "ep", q_s, q_r)

    loads[2].wait()
    loads[3].wait()
    kv_s[:, :, :HD] = dot(scaled_in, wk_v[...]).reshape(n_ep, seqs, HD)
    kv_s[:, :, HD:] = dot(scaled_in, wv_v[...]).reshape(n_ep, seqs, HD)

    for i in (14, 15, 16, 17, 18, 19, 11):
        loads[i].wait()
    gffn_row[...] = gffn_v[...].astype(F32)[None, :]
    group = rg_v[...].astype(F32)[None, :]
    id0 = group * EPG + ri_v[0:1, :].astype(F32)
    id1 = group * EPG + ri_v[1:2, :].astype(F32)
    w0, w1 = rw_v[0:1, :], rw_v[1:2, :]
    which = lax.broadcasted_iota(jnp.int32, (n_ep, batch), 0).astype(F32)
    is0, is1 = (which == id0).astype(F32), (which == id1).astype(F32)
    before = lax.broadcasted_iota(jnp.int32, (batch, batch), 0)
    after = lax.broadcasted_iota(jnp.int32, (batch, batch), 1)
    earlier = jnp.logical_and(before < after, before // seqs == after // seqs)
    rank = dot((is0 + is1).astype(BF16), earlier.astype(F32).astype(BF16))
    block_of = (lax.broadcasted_iota(jnp.int32, (1, batch), 1) // seqs).astype(F32)
    slot0 = id0 * slots + block_of * CAP + jnp.sum(rank * is0, axis=0, keepdims=True)
    slot1 = id1 * slots + block_of * CAP + jnp.sum(rank * is1, axis=0, keepdims=True)
    slot_row = lax.broadcasted_iota(jnp.int32, (slots, batch), 0).astype(F32)
    for i in range(n_ep):
        here = slot_row + float(i * slots)
        onehot_v[i] = ((here == slot0).astype(F32) + (here == slot1).astype(F32)).astype(BF16)
    mine = slot_row + (e * slots).astype(F32)
    slot_weight = jnp.sum(
        jnp.where(mine == slot0, w0, 0.0) + jnp.where(mine == slot1, w1, 0.0), axis=1, keepdims=True
    )
    row8 = lax.broadcasted_iota(jnp.int32, (128, batch), 0)
    cols = jnp.where(row8 == 0, slot0, slot1).T
    col0, col1 = cols[:, 0:1], cols[:, 1:2]
    slot_lane = lax.broadcasted_iota(jnp.int32, (batch, width), 1).astype(F32)
    for i in range(n_ep * slots // width):
        here = slot_lane + float(i * width)
        combine_v[:, i * width : (i + 1) * width] = (
            (here == col0).astype(F32) + (here == col1).astype(F32)
        ).astype(BF16)

    for i in range(n_ep):
        at = pl.ds(pl.multiple_of(i * width + (1 - core) * half, half), half)
        to_partner(WDOWN, wed.at[0, :, at], wdn_v.at[ff:, i * half : (i + 1) * half]).start()

    arrive_all(QP, "ep", q_s.at[0], q_r)
    q_sum = total(q_r, n_ep)
    inv_first = lax.rsqrt(un_hi_lo(q_sum[:, HD:]) / depth_all + EPS)
    query = (q_sum[:, :HD] * inv_first).astype(BF16)
    loads[4].wait()
    seq_row = lax.broadcasted_iota(jnp.int32, (seqs, cache_len), 0)
    place = lax.broadcasted_iota(jnp.int32, (seqs, cache_len), 1)
    scores = jnp.zeros((seqs, cache_len), F32)
    live = jnp.zeros((seqs, cache_len), jnp.int32)
    for b in range(seqs):
        scores = jnp.where(seq_row == b, dot_nt(query, k_v[b]), scores)
        live = jnp.where(seq_row == b, len_v[b], live)
    is_live = place < live
    scores = scores / math.sqrt(HD) + shift_v[0]
    tail = jnp.log1p(jnp.exp(-jnp.abs(scores)))
    soft = jnp.where(is_live, jnp.maximum(scores, 0.0) + tail, 0.0)
    running = soft
    step = 1
    while step < cache_len:
        moved = pltpu.roll(running, cache_len - step, 1)
        running = running + jnp.where(place < cache_len - step, moved, 0.0)
        step *= 2
    later = running - soft
    stick = jnp.where(is_live, jnp.exp(jnp.minimum(scores, 0.0) - tail - later), 0.0).astype(BF16)
    loads[5].wait()
    out_row = lax.broadcasted_iota(jnp.int32, (seqs, HD), 0)
    attended = jnp.zeros((seqs, HD), F32)
    for b in range(seqs):
        attended = jnp.where(out_row == b, dot(stick, v_v[b]), attended)
    att_s[...] = attended.astype(BF16)
    spread(ATT, "ep", att_s, att_r)

    loads[6].wait()
    arrive_all(ATT, "ep", att_s, att_r)
    ao_s[...] = dot(att_r[...].reshape(batch, HD), wo_v[...]).astype(BF16).reshape(n_tp, tb, width)
    scatter(AOUT, "tp", ao_s, ao_r)
    scatter(KVP, "ep", kv_s, kv_r)
    arrive_all(AOUT, "tp", ao_s.at[0], ao_r)
    own_rows = pl.ds(pl.multiple_of(t * tb, tb), tb)
    middle_own = (tok_v[own_rows, :].astype(F32) + total(ao_r, n_tp)).astype(BF16)
    mid_s[...] = middle_own
    spread(MID, "tp", mid_s, mid_r)

    arrive_all(KVP, "ep", kv_s.at[0], kv_r)
    kv_sum = total(kv_r, n_ep) * inv_first
    nk_out[...] = kv_sum[:, :HD].astype(BF16)
    nv_out[...] = kv_sum[:, HD:].astype(BF16)

    arrive_all(MID, "tp", mid_s, mid_r)
    middle = mid_r[...].reshape(batch, width)

    mid_own = mid_r[:, :, own_half].reshape(batch, half)
    mid_other = mid_r[:, :, other_half].reshape(batch, half)
    for i in range(0, n_ep, 4):
        rows = onehot_v[i : i + 4].reshape(4 * slots, batch)
        disp_s[i : i + 4] = dot(rows, mid_own).astype(BF16).reshape(4, slots, half)
    scatter(DISP, "ep", disp_s, disp_r)
    disp_o[e] = dot(onehot_v[e], mid_other).astype(BF16)

    mid_f = middle.astype(F32)
    mid_squares = jnp.sum(mid_f * mid_f, axis=1, keepdims=True)
    my_gain = gffn_row[:, pl.ds(pl.multiple_of(e * width, width), width)]
    scaled_mid = (mid_f * my_gain).astype(BF16)
    mix = jnp.sum(scaled_mid.astype(F32) * wmix_v[...].astype(F32)[None, :], axis=1, keepdims=True)
    hidden_cols = wdg_v.shape[1]
    loads[7].wait()
    loads[8].wait()
    den_s[:, :, :hidden_cols] = dot(scaled_mid, wdg_v[...]).astype(BF16).reshape(n_ep, seqs, hidden_cols)
    den_s[:, :, hidden_cols : 2 * hidden_cols] = (
        dot(scaled_mid, wdu_v[...]).astype(BF16).reshape(n_ep, seqs, hidden_cols)
    )
    lane = lax.broadcasted_iota(jnp.int32, (batch, 128), 1)
    pair = jnp.where(lane % 2 == 0, hi_lo(mix, 128), hi_lo(mid_squares, 128))
    den_s[:, :, 2 * hidden_cols :] = pair.astype(BF16).reshape(n_ep, seqs, 128)
    scatter(DENSE, "ep", den_s, den_r)

    loads[9].wait()
    loads[10].wait()

    def expert_part(ref, sources, part, carry):
        acc, sq = carry
        for src in sources:
            rows_f = ref[src].astype(F32)
            at = pl.ds(pl.multiple_of(src * width + part * half, half), half)
            scaled = (rows_f * gffn_row[:, at]).astype(BF16)
            acc = acc + dot(scaled, wgu_v[at, :])
            sq = sq + rows_f * rows_f
        return acc, sq

    def pass_on(ks):
        for k in ks:
            arrived(DISP, "ep", k, disp_s.at[0], disp_r)
            to_partner(k, disp_r.at[ep_from[k]], disp_o.at[ep_from[k]]).start()

    def passed_on(ks):
        for k in ks:
            to_partner(k, disp_r.at[ep_from[k]], disp_o.at[ep_from[k]]).wait_recv()

    near = list(range(n_ep // 2 - 1, n_ep - 1))[::-1]
    far = list(range(n_ep // 2 - 1))[::-1]
    carry = (jnp.zeros((slots, 2 * ff), F32), jnp.zeros((slots, half), F32))
    pass_on(near)
    carry = expert_part(disp_r, [e] + [ep_from[k] for k in near], core, carry)
    pass_on(far)
    passed_on(near)
    carry = expert_part(disp_o, [e] + [ep_from[k] for k in near], 1 - core, carry)
    carry = expert_part(disp_r, [ep_from[k] for k in far], core, carry)
    passed_on(far)
    acc, sq = expert_part(disp_o, [ep_from[k] for k in far], 1 - core, carry)
    inv_rows = lax.rsqrt(jnp.sum(sq, axis=1, keepdims=True) / depth_all + EPS)
    gate = acc[:, :ff] * inv_rows
    hid_s[...] = (gate / (1.0 + jnp.exp(-gate)) * (acc[:, ff:] * inv_rows)).astype(BF16)
    to_partner(HID, hid_s, hid_r).start()

    arrive_all(DENSE, "ep", den_s.at[0], den_r)
    dense = total(den_r, n_ep)
    extra = dense[:, 2 * hidden_cols :]
    mix_sum = extra[:, 0:1] + extra[:, 64:65]
    sq_sum = extra[:, 1:2] + extra[:, 65:66]
    inv_second = lax.rsqrt(sq_sum / depth_all + EPS)
    pre = dense[:, :hidden_cols] * inv_second
    lin = dense[:, hidden_cols : 2 * hidden_cols] * inv_second
    mix_gate = 1.0 / (1.0 + jnp.exp(-mix_sum * inv_second))
    dh_s[...] = (pre / (1.0 + jnp.exp(-pre)) * lin * mix_gate).astype(BF16)
    spread(DHID, "ep", dh_s, dh_r)

    pltpu.make_async_copy(wdn_v.at[:ff], wdn_v.at[:ff], down_sem).wait()
    to_partner(WDOWN, wdn_v.at[ff:], wdn_v.at[ff:]).wait_recv()
    to_partner(HID, hid_s, hid_r).wait_recv()
    hidden = jnp.concatenate([hid_s[...], hid_r[...]], axis=1)
    for i in range(0, n_ep, 4):
        rows = (dot(hidden, wdn_v[:, i * half : (i + 4) * half]) * slot_weight).astype(BF16)
        for a in range(4):
            ret_s[i + a] = rows[:, a * half : (a + 1) * half]
    scatter(RET, "ep", ret_s, ret_r)
    loads[12].wait()
    arrive_all(DHID, "ep", dh_s, dh_r)
    dense_in = dh_r[...].reshape(batch, hidden_cols)
    dp_s[...] = dot(dense_in, wdd_v[:, other_half])
    to_partner(DPART, dp_s, dp_r).start()
    part = dot(dense_in, wdd_v[:, own_half])

    arrive_all(RET, "ep", ret_s.at[0], ret_r)
    part = part + dot(combine_v[...], ret_r[...].reshape(n_ep * slots, half))
    to_partner(DPART, dp_s, dp_r).wait_recv()
    fin_s[...] = (part + dp_r[...]).astype(BF16).reshape(n_z, 2 * tb, half)
    scatter(FIN, "z", fin_s, fin_r)
    arrive_all(FIN, "z", fin_s.at[0], fin_r)
    mid_here = mid_r[pl.ds(2 * z, 2), :, own_half].reshape(2 * tb, half)
    out_s[...] = (mid_here.astype(F32) + total(fin_r, n_z)).astype(BF16)
    spread(OUT, "tp", out_s, out_r)
    arrive_all(OUT, "tp", out_s, out_r)
    for i in range(n_tp):
        at = slice(i // 2 * 2 * tb, (i // 2 + 1) * 2 * tb)
        mixed_out[at, i % 2 * half : (i % 2 + 1) * half] = out_r[i]

    sent_all(QP, "ep", q_s.at[0], q_r)
    sent_all(KVP, "ep", kv_s.at[0], kv_r)
    sent_all(ATT, "ep", att_s, att_r)
    sent_all(AOUT, "tp", ao_s.at[0], ao_r)
    sent_all(MID, "tp", mid_s, mid_r)
    sent_all(DISP, "ep", disp_s.at[0], disp_r)
    sent_all(DENSE, "ep", den_s.at[0], den_r)
    sent_all(DHID, "ep", dh_s, dh_r)
    sent_all(RET, "ep", ret_s.at[0], ret_r)
    sent_all(FIN, "z", fin_s.at[0], fin_r)
    sent_all(OUT, "tp", out_s, out_r)
    for k in range(n_ep - 1):
        to_partner(k, disp_r.at[0], disp_o.at[0]).wait_send()
    to_partner(WDOWN, wdn_v.at[ff:], wdn_v.at[ff:]).wait_send()
    to_partner(HID, hid_s, hid_r).wait_send()
    to_partner(DPART, dp_s, dp_r).wait_send()


def write_out(mixed, keys, values, mixed_out, keys_out, values_out, mixed_v, keys_v, values_v, sem):
    steps = ((mixed, mixed_v, mixed_out), (keys, keys_v, keys_out), (values, values_v, values_out))
    reads = [pltpu.make_async_copy(a, b, sem.at[i]) for i, (a, b, _) in enumerate(steps)]
    writes = [pltpu.make_async_copy(b, c, sem.at[3 + i]) for i, (_, b, c) in enumerate(steps)]
    for read in reads:
        read.start()
    for read, write in zip(reads, writes):
        read.wait()
        write.start()
    for write in writes:
        write.wait()


def on_device(n_ep, n_tp, *args):
    (
        tokens,
        gain_attn,
        w_query,
        w_key,
        w_value,
        w_output,
        key_cache,
        value_cache,
        lengths,
        score_shift,
        gain_ffn,
        w_mix,
        w_dense_gate,
        w_dense_up,
        w_dense_down,
        route_group,
        route_inner,
        route_weight,
        w_exp_gate,
        w_exp_up,
        w_exp_down,
    ) = args
    batch, width = tokens.shape
    seqs, tb = batch // n_ep, batch // n_tp
    slots, half = CAP * n_ep, width // 2
    dense_cols = w_dense_gate.shape[1]
    n = max(n_ep, n_tp)
    vmem = pl.BlockSpec(memory_space=pltpu.VMEM)
    hbm = pl.BlockSpec(memory_space=pltpu.HBM)

    def like(a, skip=0):
        return pltpu.VMEM(a.shape[skip:], a.dtype)

    def both(*shape, dtype=BF16):
        return [pltpu.VMEM(shape, dtype)] * 2

    results = pl.pallas_call(
        functools.partial(layer, n_ep, n_tp, width * n_ep),
        out_shape=(
            jax.ShapeDtypeStruct((batch, width), BF16),
            jax.ShapeDtypeStruct((seqs, HD), BF16),
            jax.ShapeDtypeStruct((seqs, HD), BF16),
        ),
        in_specs=[hbm] * 21,
        out_specs=(vmem, vmem, vmem),
        scratch_shapes=[
            like(tokens), like(w_query), like(w_key), like(w_value), like(w_output),
            like(key_cache), like(value_cache),
            like(w_dense_gate), like(w_dense_up), like(w_dense_down),
            pltpu.VMEM((w_exp_gate.shape[1], 2 * w_exp_gate.shape[2]), BF16),
            pltpu.VMEM((2 * w_exp_down.shape[1], w_exp_down.shape[2] // 2), BF16),
            like(gain_attn), pltpu.SMEM(lengths.shape, lengths.dtype),
            pltpu.SMEM(score_shift.shape, score_shift.dtype), like(gain_ffn), like(w_mix),
            like(route_group), like(route_inner.T), like(route_weight.T),
            pltpu.VMEM((1, gain_ffn.shape[0]), F32),
            pltpu.VMEM((n_ep, slots, batch), BF16),
            pltpu.VMEM((batch, n_ep * slots), BF16),
            *both(n_ep, seqs, 2 * HD),
            *both(n_ep, seqs, 2 * HD, dtype=F32),
            pltpu.VMEM((seqs, HD), BF16), pltpu.VMEM((n_ep, seqs, HD), BF16),
            *both(n_tp, tb, width),
            pltpu.VMEM((tb, width), BF16), pltpu.VMEM((n_tp, tb, width), BF16),
            *both(n_ep, slots, half), pltpu.VMEM((n_ep, slots, half), BF16),
            *both(n_ep, seqs, 2 * dense_cols + 128),
            pltpu.VMEM((seqs, dense_cols), BF16),
            pltpu.VMEM((n_ep, seqs, dense_cols), BF16),
            *both(slots, w_exp_gate.shape[2]),
            *both(n_ep, slots, half),
            *both(batch, half, dtype=F32),
            *both(n_tp // 2, 2 * tb, half),
            pltpu.VMEM((2 * tb, half), BF16), pltpu.VMEM((n_tp, 2 * tb, half), BF16),
            pltpu.SemaphoreType.DMA((20,)),
            pltpu.SemaphoreType.DMA,
            pltpu.SemaphoreType.DMA((N_PHASE, n)),
            pltpu.SemaphoreType.DMA((N_PHASE, n)),
            pltpu.SemaphoreType.DMA((N_PAIR,)),
            pltpu.SemaphoreType.DMA((N_PAIR,)),
        ],
        compiler_params=pltpu.CompilerParams(
            collective_id=0, has_side_effects=True, vmem_limit_bytes=VMEM_BYTES
        ),
        name="decode_layer",
    )(
        tokens, gain_attn, w_query, w_key, w_value, w_output, key_cache, value_cache,
        lengths, score_shift, gain_ffn, w_mix,
        w_dense_gate, w_dense_up, w_dense_down,
        route_group, route_inner.T, route_weight.T,
        w_exp_gate, w_exp_up, w_exp_down,
    )
    return pl.pallas_call(
        write_out,
        out_shape=tuple(jax.ShapeDtypeStruct(r.shape, r.dtype) for r in results),
        in_specs=[hbm] * 3,
        out_specs=(hbm, hbm, hbm),
        scratch_shapes=[*(pltpu.VMEM(r.shape, r.dtype) for r in results), pltpu.SemaphoreType.DMA((6,))],
        compiler_params=pltpu.CompilerParams(vmem_limit_bytes=VMEM_BYTES),
        name="write_out",
    )(*results)


def solution(mesh):
    placed = (
        P(None, "ep"),
        P("ep"),
        P("ep", "tp"),
        P("ep", "tp"),
        P("ep", "tp"),
        P("tp", "ep"),
        P("ep", None, "tp"),
        P("ep", None, "tp"),
        P("ep"),
        P("tp"),
        P(),
        P("ep"),
        P("ep", "tp"),
        P("ep", "tp"),
        P("tp", "ep"),
        P(),
        P(),
        P(),
        P("ep", None, "tp"),
        P("ep", None, "tp"),
        P("ep", "tp", None),
    )
    return jax.shard_map(
        functools.partial(on_device, mesh.shape["ep"], mesh.shape["tp"]),
        mesh=mesh,
        in_specs=placed,
        out_specs=(P(None, "ep"), P("ep", "tp"), P("ep", "tp")),
        check_vma=False,
    )
```
